32 devices in a mesh: ep: 4 (over y, x), tp: 8 (over z, core).
Axes of the slice: x: 2, y: 2, z: 4, core: 2. Of those that a mesh axis runs over, the one named last changes fastest.
Arguments:
- tokens: bfloat16 [768, 2048], P('ep'), may hold values from -6 to 6
- cotangent: bfloat16 [768, 2048], P('ep'), may hold values from -6 to 6
- routing: int32 [768, 2], P('ep'), may hold values from 0 to 3, all different within a row; in each aligned block of 192 rows (0 to 191, 192 to 383, ...) at most 192 rows name the same one
- gate_weights: bfloat16 [768, 2], P('ep'), may hold values from 0.19921875 to 1
- gate_proj: bfloat16 [4, 2048, 7168], P('ep', None, 'tp'), may hold values from -0.125 to 0.125
- up_proj: bfloat16 [4, 2048, 7168], P('ep', None, 'tp'), may hold values from -0.125 to 0.125
- down_proj: bfloat16 [4, 7168, 2048], P('ep', 'tp'), may hold values from -0.0625 to 0.0625
Outputs:
- grad_tokens: bfloat16 [768, 2048], P('ep', 'tp')
- grad_gates: float32 [768, 2], P('ep')
- grad_gate_proj: bfloat16 [4, 2048, 7168], P('ep', None, 'tp')
- grad_up_proj: bfloat16 [4, 2048, 7168], P('ep', None, 'tp')
- grad_down_proj: bfloat16 [4, 7168, 2048], P('ep', 'tp')
The draws below stay inside these ranges and needn't reach their ends.
Inputs may be any that keep to these rules, and one draw needn't show every extreme that they name: `routing`: each row names 2 different experts. Within each aligned block of 192 rows no expert is named by more than 192 rows, and in every draw some expert is named by exactly 192 rows of some block.
All inputs are finite; a program needn't handle non-finite values.
Results may differ from the reference program's by a relative error of at most 0.019.
Values may be sent and summed in bfloat16 or wider, within the bound.
A program may use at most 128 MiB of HBM per device.

```python
import math
import jax
import jax.numpy as jnp
import numpy as np
from jax import lax

D = 2048
FF = 7168
TOP_K = 2
TOK_DEV = 192
EXPERTS = 4
CAP = 192
TOKENS = 768
N_EP = 4


def block_scale(stream_key, shape, shards, least, high):
    def one(axis_at, shards_of):
        steps = jax.random.uniform(jax.random.fold_in(jax.random.fold_in(stream_key, 6), axis_at), (shards_of,), jnp.float32, least / len(shards), high / len(shards))
        return jnp.repeat(jnp.exp(steps), shape[axis_at] // shards_of).reshape((-1,) + (1,) * (len(shape) - axis_at - 1))

    level = one(*shards[0])
    for cut in shards[1:]:
        level = level * one(*cut)
    return level


def assign_block(rng, own, number, rows, count, top, limit, slope):
    sequence = jax.random.permutation(rng, count)
    crowded, usual = load_shares(count, rows * top, limit, slope, True), load_shares(count, rows * top, limit, slope, False)
    places = jnp.arange(count)

    def named(sizes, turn):
        used = int((sizes > 0).sum())
        fixed = max(1, used // 4)
        shifted = fixed + (places - fixed + turn * (used - fixed)) % max(1, count - fixed)
        return jnp.zeros((count,), jnp.int32).at[sequence[jnp.where(places < fixed, places, shifted)]].set(jnp.asarray(sizes, jnp.int32))

    sizes = jnp.where(number % 4 == 0, named(crowded, number // 4), named(usual, number - number // 4 - 1))
    mixed = jax.random.permutation(jax.random.fold_in(own, 3), count)
    donor, taker = mixed[0:count // 2 * 2:2], mixed[1:count // 2 * 2:2]
    room = jnp.minimum(sizes[donor] - 1, limit - sizes[taker]) // 2
    room = jnp.where((donor == sequence[0]) | (taker == sequence[0]) | (sizes[taker] == 0), 0, jnp.maximum(room, 0))
    shifted = jax.random.randint(jax.random.fold_in(own, 4), (count // 2,), 0, 1 << 20) % (room + 1)
    sizes = sizes.at[donor].add(-shifted).at[taker].add(shifted)
    items = jnp.searchsorted(jnp.cumsum(sizes), jnp.arange(rows * top), side="right").astype(jnp.int32)
    grid = items.reshape(top, rows).T
    grid = grid[jax.random.permutation(jax.random.fold_in(own, 1), rows)]
    turn = jax.random.randint(jax.random.fold_in(own, 2), (rows, 1), 0, top)
    return jnp.take_along_axis(grid, (jnp.arange(top)[None, :] + turn) % top, axis=1)


def load_shares(number_of, total, most, lean, full):
    portions = [(1 << 20) // math.isqrt(rank ** lean) + 1 for rank in range(1, number_of + 1)]
    largest = most if full else min(most, max(-(-total // number_of), total * portions[0] // sum(portions)))
    least = 1 if total - largest >= number_of - 1 else 0
    counts, surplus = [largest] + [least] * (number_of - 1), total - largest - least * (number_of - 1)
    while surplus > 0:
        free = [i for i in range(1, number_of) if counts[i] < largest] or [i for i in range(1, number_of) if counts[i] < most]
        pool, budget = sum([portions[i] for i in free]), surplus
        for i in free:
            addition = min(most - counts[i], max(1, budget * portions[i] // pool), surplus)
            counts[i] = counts[i] + addition
            surplus = surplus - addition
    return np.array(counts)


def normal_values(rng, extent, deviation, reach, cuts=(), kind=jnp.bfloat16):
    drawn = jax.random.normal(rng, extent, jnp.float32) * deviation
    if len(cuts) > 0:
        drawn = block_scale(rng, extent, cuts, -0.22, 0.18) * drawn
    return jnp.clip(drawn, min=-reach, max=reach).astype(kind)


def setup_inputs(seed: int = 0) -> dict:
    streams_of = jax.random.split(jax.random.key(seed), 8)
    tokens = normal_values(streams_of[0], (TOKENS, D), 1.0, 6.0, ((0, 4),))
    cotangent = normal_values(streams_of[1], (TOKENS, D), 1.0, 6.0, ((0, 4),))
    routing_keys = jax.random.split(jax.random.fold_in(streams_of[2], 1), TOKENS // TOK_DEV)
    routing_turns = jax.random.permutation(jax.random.fold_in(streams_of[2], 3), TOKENS // TOK_DEV)
    routing = jax.vmap(lambda own, number: assign_block(jax.random.fold_in(streams_of[2], 2), own, number, TOK_DEV, EXPERTS, TOP_K, CAP, 1))(routing_keys, routing_turns).reshape((TOKENS, TOP_K))
    gate_weights = jnp.clip(0.19921875 + 0.80078125 * jax.random.uniform(streams_of[3], (TOKENS, TOP_K), jnp.float32) ** block_scale(streams_of[3], (TOKENS, TOP_K), ((0, 4),), -0.2, 0.2), 0.19921875, 1.0).astype(jnp.bfloat16)
    gate_proj = normal_values(streams_of[4], (EXPERTS, D, FF), D ** -0.5, 0.125, ((0, 4), (2, 8)))
    up_proj = normal_values(streams_of[5], (EXPERTS, D, FF), D ** -0.5, 0.125, ((0, 4), (2, 8)))
    down_proj = normal_values(streams_of[6], (EXPERTS, FF, D), FF ** -0.5, 0.0625, ((0, 4), (1, 8)))
    return {"tokens": tokens, "cotangent": cotangent, "routing": routing, "gate_weights": gate_weights, "gate_proj": gate_proj, "up_proj": up_proj, "down_proj": down_proj}


def expert_backward(in_rows, cot_rows, gate_col, w_gate, w_up, w_down):
    gate_pre = jnp.dot(in_rows, w_gate, preferred_element_type=jnp.float32)
    up_value = jnp.dot(in_rows, w_up, preferred_element_type=jnp.float32)
    sigmoid_val = jax.nn.sigmoid(gate_pre)
    active = gate_pre * sigmoid_val
    hidden = (active * up_value).astype(jnp.bfloat16)
    contract_cols = (((1,), (1,)), ((), ()))
    contract_rows = (((0,), (0,)), ((), ()))
    back_hidden = lax.dot_general(cot_rows, w_down, contract_cols, preferred_element_type=jnp.float32)
    gate_part = jnp.sum(hidden.astype(jnp.float32) * back_hidden, axis=1)
    scaled_back = gate_col * back_hidden
    grad_pre = (scaled_back * up_value * sigmoid_val * (1.0 + gate_pre * (1.0 - sigmoid_val))).astype(jnp.bfloat16)
    grad_upval = (scaled_back * active).astype(jnp.bfloat16)
    scaled_cot = (gate_col * cot_rows.astype(jnp.float32)).astype(jnp.bfloat16)
    grad_down = lax.dot_general(hidden, scaled_cot, contract_rows, preferred_element_type=jnp.float32).astype(jnp.bfloat16)
    grad_gate = lax.dot_general(in_rows, grad_pre, contract_rows, preferred_element_type=jnp.float32).astype(jnp.bfloat16)
    grad_upw = lax.dot_general(in_rows, grad_upval, contract_rows, preferred_element_type=jnp.float32).astype(jnp.bfloat16)
    grad_in = lax.dot_general(grad_pre, w_gate, contract_cols, preferred_element_type=jnp.float32)
    grad_in = grad_in + lax.dot_general(grad_upval, w_up, contract_cols, preferred_element_type=jnp.float32)
    return grad_in, gate_part, grad_gate, grad_upw, grad_down


def reference(tokens, cotangent, routing, gate_weights, gate_proj, up_proj, down_proj):
    block_len = TOK_DEV * TOP_K
    flat_routes = routing.reshape(N_EP, block_len).astype(jnp.int32)
    onehot = (flat_routes[:, :, None] == jnp.arange(EXPERTS, dtype=jnp.int32)[None, None, :]).astype(jnp.int32)
    position = (jnp.sum(jnp.cumsum(onehot, axis=1) * onehot, axis=2) - 1).astype(jnp.int32)
    source = jnp.broadcast_to(jnp.arange(N_EP, dtype=jnp.int32)[:, None], (N_EP, block_len))
    global_index = source * block_len + jnp.arange(block_len, dtype=jnp.int32)[None, :]
    slot_owner = jnp.full((EXPERTS, N_EP, CAP), -1, jnp.int32).at[flat_routes, source, position].set(global_index)
    slot_owner = slot_owner.reshape(EXPERTS, N_EP * CAP)
    flat_gates = gate_weights.reshape(-1)

    def one_expert(inputs):
        w_gate, w_up, w_down, owner = inputs
        is_used = owner >= 0
        safe_owner = jnp.where(is_used, owner, 0)
        token_index = safe_owner // TOP_K
        in_rows = jnp.where(is_used[:, None], tokens[token_index], jnp.zeros((), jnp.bfloat16))
        cot_rows = jnp.where(is_used[:, None], cotangent[token_index], jnp.zeros((), jnp.bfloat16))
        gate_col = jnp.where(is_used, flat_gates[safe_owner].astype(jnp.float32), 0.0)[:, None]
        return expert_backward(in_rows, cot_rows, gate_col, w_gate, w_up, w_down)

    grad_in, gate_part, grad_gate, grad_upw, grad_down = lax.map(one_expert, (gate_proj, up_proj, down_proj, slot_owner))
    slot_index = (flat_routes * (N_EP * CAP) + source * CAP + position).reshape(-1)
    picked = grad_in.reshape(EXPERTS * N_EP * CAP, D)[slot_index]
    grad_tokens = jnp.sum(picked.reshape(TOKENS, TOP_K, D), axis=1).astype(jnp.bfloat16)
    grad_gates = gate_part.reshape(-1)[slot_index].reshape(TOKENS, TOP_K)
    return grad_tokens, grad_gates, grad_gate, grad_upw, grad_down
```

```python
import jax
import jax.numpy as jnp
from jax import lax
from jax.experimental import pallas as pl
from jax.experimental.pallas import tpu as pltpu
from jax.sharding import PartitionSpec as P


def expert_backward(in_rows, cot_rows, gate_col, w_gate, w_up, w_down):
    gate_pre = jnp.dot(in_rows, w_gate, preferred_element_type=jnp.float32)
    up_value = jnp.dot(in_rows, w_up, preferred_element_type=jnp.float32)
    sigmoid_val = jax.nn.sigmoid(gate_pre)
    active = gate_pre * sigmoid_val
    hidden = (active * up_value).astype(jnp.bfloat16)
    contract_cols = (((1,), (1,)), ((), ()))
    contract_rows = (((0,), (0,)), ((), ()))
    back_hidden = lax.dot_general(
        cot_rows, w_down, contract_cols, preferred_element_type=jnp.float32
    )
    gate_part = jnp.sum(hidden.astype(jnp.float32) * back_hidden, axis=1)
    scaled_back = gate_col * back_hidden
    grad_pre = (
        scaled_back * up_value * sigmoid_val * (1.0 + gate_pre * (1.0 - sigmoid_val))
    ).astype(jnp.bfloat16)
    grad_upval = (scaled_back * active).astype(jnp.bfloat16)
    scaled_cot = (gate_col * cot_rows.astype(jnp.float32)).astype(jnp.bfloat16)
    grad_down = lax.dot_general(
        hidden, scaled_cot, contract_rows, preferred_element_type=jnp.float32
    ).astype(jnp.bfloat16)
    grad_gate = lax.dot_general(
        in_rows, grad_pre, contract_rows, preferred_element_type=jnp.float32
    ).astype(jnp.bfloat16)
    grad_upw = lax.dot_general(
        in_rows, grad_upval, contract_rows, preferred_element_type=jnp.float32
    ).astype(jnp.bfloat16)
    grad_in = lax.dot_general(grad_pre, w_gate, contract_cols, preferred_element_type=jnp.float32)
    grad_in = grad_in + lax.dot_general(
        grad_upval, w_up, contract_cols, preferred_element_type=jnp.float32
    )
    return (grad_in, gate_part, grad_gate, grad_upw, grad_down)


def slotted(tokens, cotangent, routing, gate_weights, gate_proj, up_proj, down_proj):
    expert_count = lax.axis_size("ep")
    tok_rows, model_width = tokens.shape
    top_k = routing.shape[1]
    capacity = 2 * tok_rows * top_k // expert_count
    flat_routes = routing.reshape(-1)
    onehot = (flat_routes[:, None] == jnp.arange(expert_count, dtype=jnp.int32)[None, :]).astype(
        jnp.int32
    )
    position = jnp.sum(jnp.cumsum(onehot, axis=0) * onehot, axis=1) - 1
    slot_index = flat_routes * capacity + position
    slot_owner = (
        jnp.full((expert_count * capacity,), -1, jnp.int32)
        .at[slot_index]
        .set(jnp.arange(flat_routes.shape[0], dtype=jnp.int32))
    )
    is_used = slot_owner >= 0
    safe_owner = jnp.where(is_used, slot_owner, 0)
    token_index = safe_owner // top_k
    slot_gates = jnp.where(
        is_used, gate_weights.reshape(-1)[safe_owner], jnp.zeros((), jnp.bfloat16)
    )
    slot_gates = slot_gates.reshape(expert_count, capacity)

    def gather_slots(source):
        picked_rows = jnp.where(is_used[:, None], source[token_index], jnp.zeros((), jnp.bfloat16))
        return picked_rows.reshape(expert_count, capacity, source.shape[1])

    col_width = model_width // lax.axis_size("tp")
    col_start = lax.axis_index("tp") * col_width
    token_cols = lax.dynamic_slice_in_dim(tokens, col_start, col_width, 1)
    cot_cols = lax.dynamic_slice_in_dim(cotangent, col_start, col_width, 1)
    rows_part, cots_part, gates_in = (
        lax.all_to_all(gather_slots(token_cols), "ep", split_axis=0, concat_axis=0, tiled=True),
        lax.all_to_all(gather_slots(cot_cols), "ep", split_axis=0, concat_axis=0, tiled=True),
        lax.all_to_all(slot_gates, "ep", split_axis=0, concat_axis=0, tiled=True),
    )
    in_rows, cot_in = (
        lax.all_gather(rows_part, "tp", axis=2, tiled=True),
        lax.all_gather(cots_part, "tp", axis=2, tiled=True),
    )
    slot_count = in_rows.shape[0] * in_rows.shape[1]
    grad_in, gate_part, grad_gate, grad_upw, grad_down = expert_backward(
        in_rows.reshape(slot_count, model_width),
        cot_in.reshape(slot_count, model_width),
        gates_in.reshape(slot_count, 1).astype(jnp.float32),
        gate_proj[0],
        up_proj[0],
        down_proj[0],
    )
    gate_total = lax.psum(gate_part, "tp")
    grad_cols = lax.psum_scatter(
        grad_in.astype(jnp.bfloat16), "tp", scatter_dimension=1, tiled=True
    ).astype(jnp.float32)
    back_rows, back_gates = (
        lax.all_to_all(
            grad_cols.reshape(expert_count, capacity, grad_cols.shape[1]).astype(jnp.bfloat16),
            "ep",
            split_axis=0,
            concat_axis=0,
            tiled=True,
        ).astype(jnp.float32),
        lax.all_to_all(
            gate_total.reshape(expert_count, capacity).astype(jnp.bfloat16),
            "ep",
            split_axis=0,
            concat_axis=0,
            tiled=True,
        ).astype(jnp.float32),
    )
    picked = back_rows.reshape(expert_count * capacity, back_rows.shape[2])[slot_index]
    grad_tokens = jnp.sum(picked.reshape(tok_rows, top_k, picked.shape[1]), axis=1).astype(
        jnp.bfloat16
    )
    grad_gates = back_gates.reshape(-1)[slot_index].reshape(tok_rows, top_k)
    return (grad_tokens, grad_gates, grad_gate[None], grad_upw[None], grad_down[None])


MESH = pl.DeviceIdType.MESH
F32, BF16 = jnp.float32, jnp.bfloat16
NT = (((1,), (1,)), ((), ()))
TN = (((0,), (0,)), ((), ()))


def flip(index, mask):
    if mask & 1:
        index = index + 1 - 2 * (index % 2)
    if mask & 2:
        index = index + 2 - 4 * ((index // 2) % 2)
    if mask & 4:
        index = index + 4 - 8 * ((index // 4) % 2)
    return index


def lanes(start, size, unit=128):
    return pl.ds(pl.multiple_of(start, unit), size)


class Copies:
    def __init__(self, send_sem, recv_sem):
        self.send_sem, self.recv_sem, self.made = send_sem, recv_sem, []

    def send(self, src, dst, ep, tp):
        n = len(self.made)
        copy = pltpu.make_async_remote_copy(
            src_ref=src,
            dst_ref=dst,
            send_sem=self.send_sem.at[n],
            recv_sem=self.recv_sem.at[n],
            device_id=(ep, tp),
            device_id_type=MESH,
        )
        copy.start()
        self.made.append(copy)
        return copy

    def finish(self):
        for copy in self.made:
            copy.wait_send()


def layer_kernel(
    tok, cot, routing, gates, w_gate, w_up, w_down,
    out, gates_out, d_gate, d_up, d_down,
    x, c, scaled, wcat, wd, pu, hcat, hid, part,
    gs, gin, gcol, gacc, r1, m, r2, s, r3, gp, rg, gt, go,
    send_sem, recv_sem, own_sem,
):
    me, t = lax.axis_index("ep"), lax.axis_index("tp")
    core, z = t % 2, t // 2
    rows, width = tok.shape
    units = w_gate.shape[1]
    full_tiles = units // 256
    size = out.shape[1]
    eighth = width // 8
    quarter = 2 * eighth
    chunk = 2 * size
    q, far = t % 4, flip(t % 4, 2)
    other = flip(t, 1)
    blocks = {j: pl.ds(j * rows, rows) for j in range(4)}

    n = 0
    loads = []
    for src, dst in ((tok, x), (cot, c)):
        loads.append(pltpu.make_async_copy(src, dst.at[blocks[0]], own_sem.at[n]))
        n += 1
    weights = []
    for k in range(units // 128):
        for a, w in enumerate((w_gate, w_up)):
            weights.append(
                pltpu.make_async_copy(
                    w.at[:, pl.ds(128 * k, 128)],
                    wcat.at[:, pl.ds(256 * k + 128 * a, 128)],
                    own_sem.at[n],
                )
            )
            n += 1
    weights.append(pltpu.make_async_copy(w_down, wd, own_sem.at[n]))
    for copy in loads + weights:
        copy.start()

    barrier = pltpu.get_barrier_semaphore()
    partners = [(flip(me, j), t) for j in (1, 2, 3)] + [(me, flip(t, k)) for k in (1, 2, 4, 6)]
    for device in partners:
        pl.semaphore_signal(barrier, inc=1, device_id=device, device_id_type=MESH)

    gs[...] = jnp.zeros_like(gs)
    gacc[...] = jnp.zeros_like(gacc)
    routes, weight = routing[...], gates[...].astype(F32)
    for j in range(4):
        row = jnp.sum(jnp.where(routes == flip(me, j), weight, 0.0), axis=0, keepdims=True)
        gs[j, :, 0:rows] = jnp.broadcast_to(row, (8, rows))
    pl.semaphore_wait(barrier, len(partners))

    do = Copies(send_sem, recv_sem)
    for copy in loads:
        copy.wait()
    gate_in = [do.send(gs.at[j], gin.at[j], flip(me, j), t) for j in (1, 2, 3)]

    def ep_send(a, j, cols):
        ref = both[a]
        copy = do.send(ref.at[blocks[0], cols], ref.at[blocks[j], cols], flip(me, j), t)
        return (copy, a, j, cols)

    def relay(item, mask):
        piece = both[item[1]].at[blocks[item[2]], item[3]]
        return do.send(piece, piece, me, flip(t, mask))

    low, high = lanes(quarter * q, eighth), lanes(quarter * q + eighth, eighth)
    far_low, far_high = lanes(quarter * far, eighth), lanes(quarter * far + eighth, eighth)
    both = (x, c)
    near, direct = {}, {}
    for ref in (0, 1):
        near[ref] = [ep_send(ref, 1, high), ep_send(ref, 2, high)]
        near[ref] += [ep_send(ref, 3, low), ep_send(ref, 3, high)]
    for ref in (0, 1):
        direct[ref] = [ep_send(ref, j, w) for w in (low, far_low) for j in (1, 2)]
    mirror = [far_high, far_high, far_low, far_high]
    moved = ([], [])
    landed = ([], [])

    def pass_near(ref, part_of):
        for n in part_of:
            item = near[ref][n]
            item[0].wait_recv()
            moved[ref].append((relay(item, 2), ref, item[2], mirror[n]))
            landed[ref].append(relay(item, 1))

    def pass_on(items):
        for item in items:
            item[0].wait_recv()
            landed[item[1]].append(relay(item, 1))

    def gate_up(at, count):
        def tile(start, size_of):
            cols = lanes(start, size_of, 256)
            pu[at, cols] = jnp.dot(x[at, :], wcat[:, cols], preferred_element_type=F32)

        def body(k, carry):
            tile(512 * k, 512)
            return carry

        lax.fori_loop(0, full_tiles, body, 0)
        if units % 256:
            tile(512 * full_tiles, 256)

    def back_of(at, js):
        def tile(start, size_of):
            unit = lanes(start, size_of)
            back_all = lax.dot_general(c[at, :], wd[unit, :], NT, preferred_element_type=F32)
            for n, j in enumerate(js):
                mine = slice(n * rows, (n + 1) * rows)
                g = gcol[j]
                total = gacc[j, 0:rows, :]
                for k in range(size_of // 128):
                    pre = pu[blocks[j], lanes(2 * start + 256 * k, 128)]
                    up = pu[blocks[j], lanes(2 * start + 256 * k + 128, 128)]
                    back = back_all[mine, 128 * k : 128 * k + 128]
                    sig = jax.nn.sigmoid(pre)
                    act = pre * sig
                    hidden = (act * up).astype(BF16)
                    total = total + hidden.astype(F32) * back
                    scaled_back = g * back
                    grad_pre = scaled_back * up * sig * (1.0 + pre * (1.0 - sig))
                    hid[blocks[j], lanes(start + 128 * k, 128)] = hidden
                    hcat[blocks[j], lanes(2 * start + 256 * k, 128)] = grad_pre.astype(BF16)
                    hcat[blocks[j], lanes(2 * start + 256 * k + 128, 128)] = (
                        scaled_back * act
                    ).astype(BF16)
                gacc[j, 0:rows, :] = total

        def body(k, carry):
            tile(256 * k, 256)
            return carry

        lax.fori_loop(0, full_tiles, body, 0)
        if units % 256:
            tile(256 * full_tiles, 128)

    def scale(j):
        g = gcol[j][:, 0:1]
        scaled[blocks[j], :] = (g * c[blocks[j], :].astype(F32)).astype(BF16)

    def column(j, tile):
        gcol[j] = jnp.broadcast_to(tile.T[0:rows, 0:1], (rows, 128))

    base = 64

    def first(i, j):
        d = (z + 1 + i) % 4
        return pltpu.make_async_remote_copy(
            src_ref=part.at[blocks[j], lanes(chunk * d + size * (1 - core), size)],
            dst_ref=r1.at[4 * d + j],
            send_sem=send_sem.at[base + 4 * i + j],
            recv_sem=recv_sem.at[base + 4 * i + j],
            device_id=(me, other),
            device_id_type=MESH,
        )

    def grad_in(at, js):
        def body(i, carry):
            d = (z + 1 + i) % 4
            cols = lanes(chunk * d, chunk, 256)
            part[at, cols] = lax.dot_general(
                hcat[at, :], wcat[cols, :], NT, preferred_element_type=F32
            ).astype(BF16)
            for j in js:
                first(i, j).start()
            return carry

        lax.fori_loop(0, 4, body, 0)

    def second(i, j):
        d = (z + 1 + i) % 4
        return pltpu.make_async_remote_copy(
            src_ref=m.at[4 * d + j],
            dst_ref=r2.at[4 * d + j],
            send_sem=send_sem.at[base + 16 + 4 * i + j],
            recv_sem=recv_sem.at[base + 16 + 4 * i + j],
            device_id=(flip(me, j), t),
            device_id_type=MESH,
        )

    def merge(j):
        def body(i, carry):
            d = (z + 1 + i) % 4
            first(i, j).wait_recv()
            mine = part[blocks[j], lanes(chunk * d + size * core, size)].astype(F32)
            m[4 * d + j] = (mine + r1[4 * d + j].astype(F32)).astype(BF16)
            if j:
                second(i, j).start()
            return carry

        lax.fori_loop(0, 4, body, 0)

    def d_hidden(lo, hi):
        def body(i, carry):
            cols = lanes(256 * i, 256, 256)
            grads = lax.dot_general(
                x[:, cols], hcat[...], TN, preferred_element_type=F32
            ).astype(BF16)
            for k in range(units // 128):
                d_gate[cols, 128 * k : 128 * k + 128] = grads[:, 256 * k : 256 * k + 128]
                d_up[cols, 128 * k : 128 * k + 128] = grads[:, 256 * k + 128 : 256 * k + 256]
            return carry

        lax.fori_loop(lo, hi, body, 0)

    def d_out(lo, hi):
        def body(i, carry):
            cols = lanes(128 * i, 128)
            d_down[cols, :] = lax.dot_general(
                hid[:, cols], scaled[...], TN, preferred_element_type=F32
            ).astype(BF16)
            return carry

        lax.fori_loop(lo, hi, body, 0)

    column(0, gs[0])
    for copy in weights:
        copy.wait()
    gate_up(blocks[0], 1)
    pass_near(0, (0, 1))
    back_of(blocks[0], (0,))
    pass_near(0, (2, 3))
    scale(0)
    grad_in(blocks[0], (0,))
    pass_near(1, (0, 1))
    for copy in gate_in:
        copy.wait_recv()
    for j in (1, 2, 3):
        column(j, gin[j])
    merge(0)
    pass_near(1, (2, 3))
    pass_on(moved[0])
    pass_on(direct[0][0:2])
    for copy in landed[0][2:4] + landed[0][6:8]:
        copy.wait_recv()
    gate_up(blocks[3], 1)
    pass_on(direct[0][2:4])
    pass_on(moved[1][2:4])
    pass_on(direct[1][0:2])
    for copy in landed[0][0:2] + landed[0][4:6] + landed[0][8:12]:
        copy.wait_recv()
    pair = pl.ds(rows, 2 * rows)
    for copy in landed[1][2:4] + landed[1][4:6]:
        copy.wait_recv()
    back_of(blocks[3], (3,))
    scale(3)
    grad_in(blocks[3], (3,))
    pass_on(moved[1][0:2])
    pass_on(direct[1][2:4])
    gate_up(pair, 2)
    merge(3)
    for copy in landed[1][0:2] + landed[1][6:12]:
        copy.wait_recv()
    back_of(pair, (1, 2))
    scale(1)
    scale(2)
    for j in range(4):
        row = jnp.sum(gacc[j].T, axis=0, keepdims=True)
        gp[j] = jnp.broadcast_to(row, gp.shape[1:])
    stage = do.send(gp, rg.at[0], me, other)
    grad_in(pair, (1, 2))
    d_out(0, 2)
    merge(1)
    merge(2)
    stage.wait_recv()
    gt[0] = gp[...] + rg[0]
    stage = do.send(gt.at[0], rg.at[1], me, flip(t, 2))
    d_out(2, units // 128)
    stage.wait_recv()
    gt[1] = gt[0] + rg[1]
    stage = do.send(gt.at[1], rg.at[2], me, flip(t, 4))
    d_hidden(0, width // 1024)
    stage.wait_recv()
    gt[2] = gt[1] + rg[2]
    gate_back = [do.send(gt.at[2, j], go.at[j], flip(me, j), t) for j in (1, 2, 3)]
    d_hidden(width // 1024, width // 512)

    def gathered(i):
        d = (z + 1 + i) % 4
        total = m[4 * d].astype(F32)
        for j in (3, 1, 2):
            second(i, j).wait_recv()
            total = total + r2[4 * d + j].astype(F32)
        return total

    def third(i):
        d = (z + 1 + i) % 4
        return pltpu.make_async_remote_copy(
            src_ref=s.at[d],
            dst_ref=r3.at[i],
            send_sem=send_sem.at[base + 32 + i],
            recv_sem=recv_sem.at[base + 32 + i],
            device_id=(me, 2 * d + core),
            device_id_type=MESH,
        )

    for i in range(3):
        s[(z + 1 + i) % 4] = gathered(i).astype(BF16)
        third(i).start()
    total = gathered(3)
    d_hidden(width // 512, width // 256)
    for copy in gate_back:
        copy.wait_recv()
    sums = [gt[2, 0]] + [go[j] for j in (1, 2, 3)]
    picked = jnp.zeros(routing.shape, F32)
    for j in range(4):
        row = jnp.broadcast_to(sums[j][0:1, 0:rows], routing.shape)
        picked = jnp.where(routes == flip(me, j), row, picked)
    gates_out[...] = picked
    for i in range(3):
        third(i).wait_recv()
        total = total + r3[i].astype(F32)
    out[...] = total.astype(out.dtype)
    do.finish()
    for i in range(4):
        for j in range(4):
            first(i, j).wait_send()
            if j:
                second(i, j).wait_send()
        if i < 3:
            third(i).wait_send()


def dense(tokens, cotangent, routing, gate_weights, gate_proj, up_proj, down_proj):
    rows, width = tokens.shape
    units, parts = gate_proj.shape[2], lax.axis_size("tp")
    size = width // parts
    top_k = routing.shape[1]
    vmem, anywhere = pl.BlockSpec(memory_space=pltpu.VMEM), pl.BlockSpec(memory_space=pl.ANY)
    shape = jax.ShapeDtypeStruct
    tile = pltpu.VMEM((16, rows, size), BF16)
    flat = (4, 8, 256)
    grad_tokens, grad_gates, d_gate, d_up, d_down = pl.pallas_call(
        layer_kernel,
        out_shape=[
            shape((rows, size), BF16),
            shape((top_k, rows), F32),
            shape((width, units), BF16),
            shape((width, units), BF16),
            shape((units, width), BF16),
        ],
        in_specs=[anywhere, anywhere, vmem, vmem, anywhere, anywhere, anywhere],
        out_specs=[vmem] * 5,
        scratch_shapes=[
            pltpu.VMEM((4 * rows, width), BF16),
            pltpu.VMEM((4 * rows, width), BF16),
            pltpu.VMEM((4 * rows, width), BF16),
            pltpu.VMEM((width, 2 * units), BF16),
            pltpu.VMEM((units, width), BF16),
            pltpu.VMEM((4 * rows, 2 * units), F32),
            pltpu.VMEM((4 * rows, 2 * units), BF16),
            pltpu.VMEM((4 * rows, units), BF16),
            pltpu.VMEM((4 * rows, width), BF16),
            pltpu.VMEM(flat, F32),
            pltpu.VMEM(flat, F32),
            pltpu.VMEM((4, rows, 128), F32),
            pltpu.VMEM((4, 256, 128), F32),
            tile,
            tile,
            tile,
            pltpu.VMEM((4, rows, size), BF16),
            pltpu.VMEM((3, rows, size), BF16),
            pltpu.VMEM(flat, F32),
            pltpu.VMEM((3,) + flat, F32),
            pltpu.VMEM((3,) + flat, F32),
            pltpu.VMEM(flat, F32),
            pltpu.SemaphoreType.DMA((104,)),
            pltpu.SemaphoreType.DMA((104,)),
            pltpu.SemaphoreType.DMA((3 + 2 * (units // 128),)),
        ],
        compiler_params=pltpu.CompilerParams(
            collective_id=0, has_side_effects=True, vmem_limit_bytes=62 << 20
        ),
    )(tokens, cotangent, routing.T, gate_weights.T, gate_proj[0], up_proj[0], down_proj[0])
    return grad_tokens, grad_gates.T, d_gate[None], d_up[None], d_down[None]


def local(tokens, cotangent, routing, gate_weights, gate_proj, up_proj, down_proj):
    experts, parts = lax.axis_size("ep"), lax.axis_size("tp")
    capacity = 2 * tokens.shape[0] * routing.shape[1] // experts
    fits = experts == 4 and parts == 8 and tokens.shape[1] % 1024 == 0
    fits = fits and tokens.shape[0] % 16 == 0 and tokens.shape[0] <= 256
    fits = fits and gate_proj.shape[2] % 128 == 0
    plan = dense if capacity >= tokens.shape[0] and fits else slotted
    return plan(tokens, cotangent, routing, gate_weights, gate_proj, up_proj, down_proj)


def solution(mesh):
    return jax.shard_map(
        local,
        mesh=mesh,
        in_specs=(
            P("ep", None),
            P("ep", None),
            P("ep", None),
            P("ep", None),
            P("ep", None, "tp"),
            P("ep", None, "tp"),
            P("ep", "tp", None),
        ),
        out_specs=(
            P("ep", "tp"),
            P("ep", None),
            P("ep", None, "tp"),
            P("ep", None, "tp"),
            P("ep", "tp", None),
        ),
        check_vma=False,
    )
```

```python
import jax
import jax.numpy as jnp
from jax import lax
from jax.experimental import pallas as pl
from jax.experimental.pallas import tpu as pltpu
from jax.sharding import PartitionSpec as P


def expert_backward(in_rows, cot_rows, gate_col, w_gate, w_up, w_down):
    gate_pre = jnp.dot(in_rows, w_gate, preferred_element_type=jnp.float32)
    up_value = jnp.dot(in_rows, w_up, preferred_element_type=jnp.float32)
    sigmoid_val = jax.nn.sigmoid(gate_pre)
    active = gate_pre * sigmoid_val
    hidden = (active * up_value).astype(jnp.bfloat16)
    contract_cols = (((1,), (1,)), ((), ()))
    contract_rows = (((0,), (0,)), ((), ()))
    back_hidden = lax.dot_general(
        cot_rows, w_down, contract_cols, preferred_element_type=jnp.float32
    )
    gate_part = jnp.sum(hidden.astype(jnp.float32) * back_hidden, axis=1)
    scaled_back = gate_col * back_hidden
    grad_pre = (
        scaled_back * up_value * sigmoid_val * (1.0 + gate_pre * (1.0 - sigmoid_val))
    ).astype(jnp.bfloat16)
    grad_upval = (scaled_back * active).astype(jnp.bfloat16)
    scaled_cot = (gate_col * cot_rows.astype(jnp.float32)).astype(jnp.bfloat16)
    grad_down = lax.dot_general(
        hidden, scaled_cot, contract_rows, preferred_element_type=jnp.float32
    ).astype(jnp.bfloat16)
    grad_gate = lax.dot_general(
        in_rows, grad_pre, contract_rows, preferred_element_type=jnp.float32
    ).astype(jnp.bfloat16)
    grad_upw = lax.dot_general(
        in_rows, grad_upval, contract_rows, preferred_element_type=jnp.float32
    ).astype(jnp.bfloat16)
    grad_in = lax.dot_general(grad_pre, w_gate, contract_cols, preferred_element_type=jnp.float32)
    grad_in = grad_in + lax.dot_general(
        grad_upval, w_up, contract_cols, preferred_element_type=jnp.float32
    )
    return (grad_in, gate_part, grad_gate, grad_upw, grad_down)


def slotted(tokens, cotangent, routing, gate_weights, gate_proj, up_proj, down_proj):
    expert_count = lax.axis_size("ep")
    tok_rows, model_width = tokens.shape
    top_k = routing.shape[1]
    capacity = 2 * tok_rows * top_k // expert_count
    flat_routes = routing.reshape(-1)
    onehot = (flat_routes[:, None] == jnp.arange(expert_count, dtype=jnp.int32)[None, :]).astype(
        jnp.int32
    )
    position = jnp.sum(jnp.cumsum(onehot, axis=0) * onehot, axis=1) - 1
    slot_index = flat_routes * capacity + position
    slot_owner = (
        jnp.full((expert_count * capacity,), -1, jnp.int32)
        .at[slot_index]
        .set(jnp.arange(flat_routes.shape[0], dtype=jnp.int32))
    )
    is_used = slot_owner >= 0
    safe_owner = jnp.where(is_used, slot_owner, 0)
    token_index = safe_owner // top_k
    slot_gates = jnp.where(
        is_used, gate_weights.reshape(-1)[safe_owner], jnp.zeros((), jnp.bfloat16)
    )
    slot_gates = slot_gates.reshape(expert_count, capacity)

    def gather_slots(source):
        picked_rows = jnp.where(is_used[:, None], source[token_index], jnp.zeros((), jnp.bfloat16))
        return picked_rows.reshape(expert_count, capacity, source.shape[1])

    col_width = model_width // lax.axis_size("tp")
    col_start = lax.axis_index("tp") * col_width
    token_cols = lax.dynamic_slice_in_dim(tokens, col_start, col_width, 1)
    cot_cols = lax.dynamic_slice_in_dim(cotangent, col_start, col_width, 1)
    rows_part, cots_part, gates_in = (
        lax.all_to_all(gather_slots(token_cols), "ep", split_axis=0, concat_axis=0, tiled=True),
        lax.all_to_all(gather_slots(cot_cols), "ep", split_axis=0, concat_axis=0, tiled=True),
        lax.all_to_all(slot_gates, "ep", split_axis=0, concat_axis=0, tiled=True),
    )
    in_rows, cot_in = (
        lax.all_gather(rows_part, "tp", axis=2, tiled=True),
        lax.all_gather(cots_part, "tp", axis=2, tiled=True),
    )
    slot_count = in_rows.shape[0] * in_rows.shape[1]
    grad_in, gate_part, grad_gate, grad_upw, grad_down = expert_backward(
        in_rows.reshape(slot_count, model_width),
        cot_in.reshape(slot_count, model_width),
        gates_in.reshape(slot_count, 1).astype(jnp.float32),
        gate_proj[0],
        up_proj[0],
        down_proj[0],
    )
    gate_total = lax.psum(gate_part, "tp")
    grad_cols = lax.psum_scatter(
        grad_in.astype(jnp.bfloat16), "tp", scatter_dimension=1, tiled=True
    ).astype(jnp.float32)
    back_rows, back_gates = (
        lax.all_to_all(
            grad_cols.reshape(expert_count, capacity, grad_cols.shape[1]).astype(jnp.bfloat16),
            "ep",
            split_axis=0,
            concat_axis=0,
            tiled=True,
        ).astype(jnp.float32),
        lax.all_to_all(
            gate_total.reshape(expert_count, capacity).astype(jnp.bfloat16),
            "ep",
            split_axis=0,
            concat_axis=0,
            tiled=True,
        ).astype(jnp.float32),
    )
    picked = back_rows.reshape(expert_count * capacity, back_rows.shape[2])[slot_index]
    grad_tokens = jnp.sum(picked.reshape(tok_rows, top_k, picked.shape[1]), axis=1).astype(
        jnp.bfloat16
    )
    grad_gates = back_gates.reshape(-1)[slot_index].reshape(tok_rows, top_k)
    return (grad_tokens, grad_gates, grad_gate[None], grad_upw[None], grad_down[None])


MESH = pl.DeviceIdType.MESH
F32, BF16 = jnp.float32, jnp.bfloat16
NT = (((1,), (1,)), ((), ()))
TN = (((0,), (0,)), ((), ()))


def flip(index, mask):
    if mask & 1:
        index = index + 1 - 2 * (index % 2)
    if mask & 2:
        index = index + 2 - 4 * ((index // 2) % 2)
    if mask & 4:
        index = index + 4 - 8 * ((index // 4) % 2)
    return index


def lanes(start, size, unit=128):
    return pl.ds(pl.multiple_of(start, unit), size)


class Copies:
    def __init__(self, send_sem, recv_sem):
        self.send_sem, self.recv_sem, self.made = send_sem, recv_sem, []

    def send(self, src, dst, ep, tp):
        n = len(self.made)
        copy = pltpu.make_async_remote_copy(
            src_ref=src,
            dst_ref=dst,
            send_sem=self.send_sem.at[n],
            recv_sem=self.recv_sem.at[n],
            device_id=(ep, tp),
            device_id_type=MESH,
        )
        copy.start()
        self.made.append(copy)
        return copy

    def finish(self):
        for copy in self.made:
            copy.wait_send()


def layer_kernel(
    tok, cot, routing, gates, w_gate, w_up, w_down,
    out, gates_out, d_gate, d_up, d_down,
    routes_in, weight_in, x, c, scaled, wcat, wd, pu, hcat, hid, part,
    gs, gin, gcol, gacc, r1, m, r2, r4, s, r3, gp, rg, gt, go,
    send_sem, recv_sem, own_sem,
):
    me, t = lax.axis_index("ep"), lax.axis_index("tp")
    core, z = t % 2, t // 2
    rows, width = tok.shape
    units = w_gate.shape[1]
    full_tiles = units // 256
    size = out.shape[1]
    eighth = width // 8
    quarter = 2 * eighth
    chunk = 2 * size
    q, far = t % 4, flip(t % 4, 2)
    other = flip(t, 1)
    blocks = {j: pl.ds(j * rows, rows) for j in range(4)}

    n = 0
    loads = []
    for src, dst in (
        (tok, x.at[blocks[0]]),
        (cot, c.at[blocks[0]]),
        (routing, routes_in),
        (gates, weight_in),
    ):
        loads.append(pltpu.make_async_copy(src, dst, own_sem.at[n]))
        n += 1
    weights = []
    for k in range(units // 128):
        for a, w in enumerate((w_gate, w_up)):
            weights.append(
                pltpu.make_async_copy(
                    w.at[:, pl.ds(128 * k, 128)],
                    wcat.at[:, pl.ds(256 * k + 128 * a, 128)],
                    own_sem.at[n],
                )
            )
            n += 1
    weights.append(pltpu.make_async_copy(w_down, wd, own_sem.at[n]))
    for copy in loads + weights:
        copy.start()

    barrier = pltpu.get_barrier_semaphore()
    partners = [(flip(me, j), t) for j in (1, 2, 3)] + [(me, flip(t, k)) for k in (1, 2, 4, 6)]
    for device in partners:
        pl.semaphore_signal(barrier, inc=1, device_id=device, device_id_type=MESH)

    gs[...] = jnp.zeros_like(gs)
    gacc[...] = jnp.zeros_like(gacc)
    for copy in loads:
        copy.wait()
    routes, weight = routes_in[...], weight_in[...].astype(F32)
    for j in range(4):
        row = jnp.sum(jnp.where(routes == flip(me, j), weight, 0.0), axis=0, keepdims=True)
        gs[j, :, 0:rows] = jnp.broadcast_to(row, (8, rows))
    pl.semaphore_wait(barrier, len(partners))

    do = Copies(send_sem, recv_sem)
    gate_in = [do.send(gs.at[j], gin.at[j], flip(me, j), t) for j in (1, 2, 3)]

    def ep_send(a, j, cols):
        ref = both[a]
        copy = do.send(ref.at[blocks[0], cols], ref.at[blocks[j], cols], flip(me, j), t)
        return (copy, a, j, cols)

    def relay(item, mask):
        piece = both[item[1]].at[blocks[item[2]], item[3]]
        return do.send(piece, piece, me, flip(t, mask))

    low, high = lanes(quarter * q, eighth), lanes(quarter * q + eighth, eighth)
    far_low, far_high = lanes(quarter * far, eighth), lanes(quarter * far + eighth, eighth)
    both = (x, c)
    lead, rest, wide = {}, {}, {}
    landed = {0: [], 1: [], 2: [], 3: []}

    def over_ep(item, j):
        _, a, _, cols = item
        src = both[a].at[blocks[item[2]], cols]
        copy = do.send(src, both[a].at[blocks[3], cols], flip(me, j), t)
        return (copy, a, 3, cols)

    def over_z(item, mirror):
        return (relay(item, 2), item[1], item[2], mirror)

    def pass_on(items):
        for item in items:
            item[0].wait_recv()
            landed[item[2]].append((item[1], relay(item, 1)))

    def complete(j, a):
        for kind, copy in landed[j]:
            if kind == a:
                copy.wait_recv()

    for a in (0, 1):
        lead[a] = [ep_send(a, 1, low), ep_send(a, 2, high)]
    rest[0] = [ep_send(0, 1, high), ep_send(0, 2, low)]

    def gate_up(at, count):
        def tile(start, size_of):
            cols = lanes(start, size_of, 256)
            pu[at, cols] = jnp.dot(x[at, :], wcat[:, cols], preferred_element_type=F32)

        def body(k, carry):
            tile(512 * k, 512)
            return carry

        lax.fori_loop(0, full_tiles, body, 0)
        if units % 256:
            tile(512 * full_tiles, 256)

    def back_of(at, js):
        def tile(start, size_of):
            unit = lanes(start, size_of)
            back_all = lax.dot_general(c[at, :], wd[unit, :], NT, preferred_element_type=F32)
            for n, j in enumerate(js):
                mine = slice(n * rows, (n + 1) * rows)
                g = gcol[j]
                total = gacc[j, 0:rows, :]
                for k in range(size_of // 128):
                    pre = pu[blocks[j], lanes(2 * start + 256 * k, 128)]
                    up = pu[blocks[j], lanes(2 * start + 256 * k + 128, 128)]
                    back = back_all[mine, 128 * k : 128 * k + 128]
                    sig = jax.nn.sigmoid(pre)
                    act = pre * sig
                    hidden = (act * up).astype(BF16)
                    total = total + hidden.astype(F32) * back
                    scaled_back = g * back
                    grad_pre = scaled_back * up * sig * (1.0 + pre * (1.0 - sig))
                    hid[blocks[j], lanes(start + 128 * k, 128)] = hidden
                    hcat[blocks[j], lanes(2 * start + 256 * k, 128)] = grad_pre.astype(BF16)
                    hcat[blocks[j], lanes(2 * start + 256 * k + 128, 128)] = (
                        scaled_back * act
                    ).astype(BF16)
                gacc[j, 0:rows, :] = total

        def body(k, carry):
            tile(256 * k, 256)
            return carry

        lax.fori_loop(0, full_tiles, body, 0)
        if units % 256:
            tile(256 * full_tiles, 128)

    def scale(j):
        g = gcol[j][:, 0:1]
        scaled[blocks[j], :] = (g * c[blocks[j], :].astype(F32)).astype(BF16)

    def column(j, tile):
        gcol[j] = jnp.broadcast_to(tile.T[0:rows, 0:1], (rows, 128))

    base = 64

    def first(i, j):
        d = (z + 1 + i) % 4
        return pltpu.make_async_remote_copy(
            src_ref=part.at[blocks[j], lanes(chunk * d + size * (1 - core), size)],
            dst_ref=r1.at[4 * d + j],
            send_sem=send_sem.at[base + 4 * i + j],
            recv_sem=recv_sem.at[base + 4 * i + j],
            device_id=(me, other),
            device_id_type=MESH,
        )

    def grad_in(at, js):
        def body(i, carry):
            d = (z + 1 + i) % 4
            cols = lanes(chunk * d, chunk, 256)
            part[at, cols] = lax.dot_general(
                hcat[at, :], wcat[cols, :], NT, preferred_element_type=F32
            ).astype(BF16)
            for j in js:
                first(i, j).start()
            return carry

        lax.fori_loop(0, 4, body, 0)

    def second(i, j):
        d = (z + 1 + i) % 4
        return pltpu.make_async_remote_copy(
            src_ref=m.at[4 * d + j],
            dst_ref=r2.at[4 * d + j],
            send_sem=send_sem.at[base + 16 + 4 * i + j],
            recv_sem=recv_sem.at[base + 16 + 4 * i + j],
            device_id=(flip(me, j), t),
            device_id_type=MESH,
        )

    def fourth(d):
        return pltpu.make_async_remote_copy(
            src_ref=m.at[4 * d + 3],
            dst_ref=r4.at[d // 2],
            send_sem=send_sem.at[base + 36 + d],
            recv_sem=recv_sem.at[base + 36 + d],
            device_id=(me, flip(t, 2)),
            device_id_type=MESH,
        )

    def merge_diagonal():
        for i in (0, 2, 1, 3):
            d = (z + 1 + i) % 4
            first(i, 3).wait_recv()
            mine = part[blocks[3], lanes(chunk * d + size * core, size)].astype(F32)
            m[4 * d + 3] = (mine + r1[4 * d + 3].astype(F32)).astype(BF16)
            if i % 2 == 0:
                fourth(d).start()

    def send_diagonal():
        for i in (1, 3):
            d = (z + 1 + i) % 4
            fourth(d).wait_recv()
            m[4 * d + 3] = (m[4 * d + 3].astype(F32) + r4[d // 2].astype(F32)).astype(BF16)
            second(i, 3).start()

    def merge(j):
        def body(i, carry):
            d = (z + 1 + i) % 4
            first(i, j).wait_recv()
            mine = part[blocks[j], lanes(chunk * d + size * core, size)].astype(F32)
            m[4 * d + j] = (mine + r1[4 * d + j].astype(F32)).astype(BF16)
            if j:
                second(i, j).start()
            return carry

        lax.fori_loop(0, 4, body, 0)

    def d_hidden(lo, hi):
        def body(i, carry):
            cols = lanes(256 * i, 256, 256)
            grads = lax.dot_general(
                x[:, cols], hcat[...], TN, preferred_element_type=F32
            ).astype(BF16)
            for k in range(units // 128):
                d_gate[cols, 128 * k : 128 * k + 128] = grads[:, 256 * k : 256 * k + 128]
                d_up[cols, 128 * k : 128 * k + 128] = grads[:, 256 * k + 128 : 256 * k + 256]
            return carry

        lax.fori_loop(lo, hi, body, 0)

    def d_out(lo, hi):
        def body(i, carry):
            cols = lanes(128 * i, 128)
            d_down[cols, :] = lax.dot_general(
                hid[:, cols], scaled[...], TN, preferred_element_type=F32
            ).astype(BF16)
            return carry

        lax.fori_loop(lo, hi, body, 0)

    column(0, gs[0])
    for copy in weights:
        copy.wait()
    gate_up(blocks[0], 1)
    pass_on(lead[0])
    diag = {0: [over_ep(lead[0][0], 2), over_ep(lead[0][1], 1)]}
    crossed = {0: [over_z(lead[0][0], far_low), over_z(lead[0][1], far_high)]}
    back_of(blocks[0], (0,))
    pass_on(lead[1])
    diag[1] = [over_ep(lead[1][0], 2), over_ep(lead[1][1], 1)]
    crossed[1] = [over_z(lead[1][0], far_low)]
    wide[0] = [ep_send(0, 1, far_high), ep_send(0, 2, far_low)]
    rest[1] = [ep_send(1, 1, high), ep_send(1, 2, low)]
    wide[1] = [ep_send(1, 1, far_high), ep_send(1, 2, far_low)]
    scale(0)
    grad_in(blocks[0], (0,))
    pass_on(rest[0])
    pass_on(crossed[0])
    pass_on(diag[0])
    across = {0: [over_z(diag[0][0], far_low), over_z(diag[0][1], far_high)]}
    merge(0)
    for copy in gate_in:
        copy.wait_recv()
    for j in (1, 2, 3):
        column(j, gin[j])
    pass_on(diag[1])
    across[1] = [over_z(diag[1][0], far_low), over_z(diag[1][1], far_high)]
    crossed[1].append(over_z(lead[1][1], far_high))
    pass_on(wide[0])
    pass_on(crossed[1][0:1])
    complete(1, 0)
    complete(2, 0)
    pair = pl.ds(rows, 2 * rows)
    gate_up(pair, 2)
    pass_on(rest[1])
    pass_on(across[0])
    complete(3, 0)
    gate_up(blocks[3], 1)
    pass_on(wide[1])
    complete(1, 1)
    back_of(blocks[1], (1,))
    scale(1)
    pass_on(across[1])
    complete(3, 1)
    back_of(blocks[3], (3,))
    scale(3)
    pass_on(crossed[1][1:2])
    grad_in(blocks[3], (3,))
    complete(2, 1)
    back_of(blocks[2], (2,))
    merge_diagonal()
    grad_in(pair, (1, 2))
    send_diagonal()
    scale(2)
    merge(1)
    merge(2)
    for j in range(4):
        row = jnp.sum(gacc[j].T, axis=0, keepdims=True)
        gp[j] = jnp.broadcast_to(row, gp.shape[1:])
    stage = do.send(gp, rg.at[0], me, other)
    d_out(0, 3)
    stage.wait_recv()
    gt[0] = gp[...] + rg[0]
    stage = do.send(gt.at[0], rg.at[1], me, flip(t, 2))
    d_out(3, units // 128)
    stage.wait_recv()
    gt[1] = gt[0] + rg[1]
    stage = do.send(gt.at[1], rg.at[2], me, flip(t, 4))
    d_hidden(0, width // 1024)
    stage.wait_recv()
    gt[2] = gt[1] + rg[2]
    gate_back = [do.send(gt.at[2, j], go.at[j], flip(me, j), t) for j in (1, 2, 3)]

    def gathered(i):
        d = (z + 1 + i) % 4
        total = m[4 * d].astype(F32)
        for j in (3, 1, 2) if i % 2 else (1, 2):
            second(i, j).wait_recv()
            total = total + r2[4 * d + j].astype(F32)
        return total

    def third(i):
        d = (z + 1 + i) % 4
        return pltpu.make_async_remote_copy(
            src_ref=s.at[d],
            dst_ref=r3.at[i],
            send_sem=send_sem.at[base + 32 + i],
            recv_sem=recv_sem.at[base + 32 + i],
            device_id=(me, 2 * d + core),
            device_id_type=MESH,
        )

    for i in range(3):
        s[(z + 1 + i) % 4] = gathered(i).astype(BF16)
        third(i).start()
    d_hidden(width // 1024, width // 256)
    total = gathered(3)
    for copy in gate_back:
        copy.wait_recv()
    sums = [gt[2, 0]] + [go[j] for j in (1, 2, 3)]
    picked = jnp.zeros(routing.shape, F32)
    for j in range(4):
        row = jnp.broadcast_to(sums[j][0:1, 0:rows], routing.shape)
        picked = jnp.where(routes == flip(me, j), row, picked)
    gates_out[...] = picked
    for i in range(3):
        third(i).wait_recv()
        total = total + r3[i].astype(F32)
    out[...] = total.astype(out.dtype)
    do.finish()
    for i in range(4):
        for j in range(4):
            first(i, j).wait_send()
            if j in (1, 2) or (j and i % 2):
                second(i, j).wait_send()
        if i % 2 == 0:
            fourth((z + 1 + i) % 4).wait_send()
        if i < 3:
            third(i).wait_send()


def store_kernel(*refs):
    sources, targets, sem = refs[0:5], refs[5:10], refs[10]
    copies = []
    for a, (src, dst) in enumerate(zip(sources, targets)):
        parts = 4 if src.shape[0] % 512 == 0 or src.shape[0] > 512 else 1
        step = src.shape[0] // parts
        for k in range(parts):
            piece = pl.ds(k * step, step)
            copies.append(pltpu.make_async_copy(src.at[piece], dst.at[piece], sem.at[a, k]))
    for copy in copies:
        copy.start()
    for copy in copies:
        copy.wait()


def dense(tokens, cotangent, routing, gate_weights, gate_proj, up_proj, down_proj):
    rows, width = tokens.shape
    units, parts = gate_proj.shape[2], lax.axis_size("tp")
    size = width // parts
    top_k = routing.shape[1]
    vmem, hbm = pl.BlockSpec(memory_space=pltpu.VMEM), pl.BlockSpec(memory_space=pltpu.HBM)
    shape = jax.ShapeDtypeStruct
    tile = pltpu.VMEM((16, rows, size), BF16)
    flat = (4, 8, 256)
    results = pl.pallas_call(
        layer_kernel,
        out_shape=[
            pltpu.VMEM((rows, size), BF16),
            pltpu.VMEM((top_k, rows), F32),
            pltpu.VMEM((width, units), BF16),
            pltpu.VMEM((width, units), BF16),
            pltpu.VMEM((units, width), BF16),
        ],
        in_specs=[hbm] * 7,
        out_specs=[vmem] * 5,
        scratch_shapes=[
            pltpu.VMEM((top_k, rows), routing.dtype),
            pltpu.VMEM((top_k, rows), gate_weights.dtype),
            pltpu.VMEM((4 * rows, width), BF16),
            pltpu.VMEM((4 * rows, width), BF16),
            pltpu.VMEM((4 * rows, width), BF16),
            pltpu.VMEM((width, 2 * units), BF16),
            pltpu.VMEM((units, width), BF16),
            pltpu.VMEM((4 * rows, 2 * units), F32),
            pltpu.VMEM((4 * rows, 2 * units), BF16),
            pltpu.VMEM((4 * rows, units), BF16),
            pltpu.VMEM((4 * rows, width), BF16),
            pltpu.VMEM(flat, F32),
            pltpu.VMEM(flat, F32),
            pltpu.VMEM((4, rows, 128), F32),
            pltpu.VMEM((4, 256, 128), F32),
            tile,
            tile,
            tile,
            pltpu.VMEM((2, rows, size), BF16),
            pltpu.VMEM((4, rows, size), BF16),
            pltpu.VMEM((3, rows, size), BF16),
            pltpu.VMEM(flat, F32),
            pltpu.VMEM((3,) + flat, F32),
            pltpu.VMEM((3,) + flat, F32),
            pltpu.VMEM(flat, F32),
            pltpu.SemaphoreType.DMA((104,)),
            pltpu.SemaphoreType.DMA((104,)),
            pltpu.SemaphoreType.DMA((5 + 2 * (units // 128),)),
        ],
        compiler_params=pltpu.CompilerParams(
            collective_id=0, has_side_effects=True, vmem_limit_bytes=42 << 20
        ),
    )(
        *(
            pltpu.with_memory_space_constraint(a, pltpu.HBM)
            for a in (
                tokens,
                cotangent,
                routing.T,
                gate_weights.T,
                gate_proj[0],
                up_proj[0],
                down_proj[0],
            )
        )
    )
    grad_tokens, grad_gates, d_gate, d_up, d_down = pl.pallas_call(
        store_kernel,
        out_shape=[shape(r.shape, r.dtype) for r in results],
        in_specs=[vmem] * 5,
        out_specs=[hbm] * 5,
        scratch_shapes=[pltpu.SemaphoreType.DMA((5, 4))],
        compiler_params=pltpu.CompilerParams(vmem_limit_bytes=1 << 20),
    )(*results)
    return grad_tokens, grad_gates.T, d_gate[None], d_up[None], d_down[None]


def local(tokens, cotangent, routing, gate_weights, gate_proj, up_proj, down_proj):
    experts, parts = lax.axis_size("ep"), lax.axis_size("tp")
    capacity = 2 * tokens.shape[0] * routing.shape[1] // experts
    fits = experts == 4 and parts == 8 and tokens.shape[1] % 1024 == 0
    fits = fits and tokens.shape[0] % 16 == 0 and tokens.shape[0] <= 256
    fits = fits and gate_proj.shape[2] % 128 == 0
    plan = dense if capacity >= tokens.shape[0] and fits else slotted
    return plan(tokens, cotangent, routing, gate_weights, gate_proj, up_proj, down_proj)


def solution(mesh):
    return jax.shard_map(
        local,
        mesh=mesh,
        in_specs=(
            P("ep", None),
            P("ep", None),
            P("ep", None),
            P("ep", None),
            P("ep", None, "tp"),
            P("ep", None, "tp"),
            P("ep", "tp", None),
        ),
        out_specs=(
            P("ep", "tp"),
            P("ep", None),
            P("ep", None, "tp"),
            P("ep", None, "tp"),
            P("ep", "tp", None),
        ),
        check_vma=False,
    )
```

```python
import jax
import jax.numpy as jnp
from jax import lax
from jax.experimental import pallas as pl
from jax.experimental.pallas import tpu as pltpu
from jax.sharding import PartitionSpec as P


def expert_backward(in_rows, cot_rows, gate_col, w_gate, w_up, w_down):
    gate_pre = jnp.dot(in_rows, w_gate, preferred_element_type=jnp.float32)
    up_value = jnp.dot(in_rows, w_up, preferred_element_type=jnp.float32)
    sigmoid_val = jax.nn.sigmoid(gate_pre)
    active = gate_pre * sigmoid_val
    hidden = (active * up_value).astype(jnp.bfloat16)
    contract_cols = (((1,), (1,)), ((), ()))
    contract_rows = (((0,), (0,)), ((), ()))
    back_hidden = lax.dot_general(
        cot_rows, w_down, contract_cols, preferred_element_type=jnp.float32
    )
    gate_part = jnp.sum(hidden.astype(jnp.float32) * back_hidden, axis=1)
    scaled_back = gate_col * back_hidden
    grad_pre = (
        scaled_back * up_value * sigmoid_val * (1.0 + gate_pre * (1.0 - sigmoid_val))
    ).astype(jnp.bfloat16)
    grad_upval = (scaled_back * active).astype(jnp.bfloat16)
    scaled_cot = (gate_col * cot_rows.astype(jnp.float32)).astype(jnp.bfloat16)
    grad_down = lax.dot_general(
        hidden, scaled_cot, contract_rows, preferred_element_type=jnp.float32
    ).astype(jnp.bfloat16)
    grad_gate = lax.dot_general(
        in_rows, grad_pre, contract_rows, preferred_element_type=jnp.float32
    ).astype(jnp.bfloat16)
    grad_upw = lax.dot_general(
        in_rows, grad_upval, contract_rows, preferred_element_type=jnp.float32
    ).astype(jnp.bfloat16)
    grad_in = lax.dot_general(grad_pre, w_gate, contract_cols, preferred_element_type=jnp.float32)
    grad_in = grad_in + lax.dot_general(
        grad_upval, w_up, contract_cols, preferred_element_type=jnp.float32
    )
    return (grad_in, gate_part, grad_gate, grad_upw, grad_down)


def slotted(tokens, cotangent, routing, gate_weights, gate_proj, up_proj, down_proj):
    expert_count = lax.axis_size("ep")
    tok_rows, model_width = tokens.shape
    top_k = routing.shape[1]
    capacity = 2 * tok_rows * top_k // expert_count
    flat_routes = routing.reshape(-1)
    onehot = (flat_routes[:, None] == jnp.arange(expert_count, dtype=jnp.int32)[None, :]).astype(
        jnp.int32
    )
    position = jnp.sum(jnp.cumsum(onehot, axis=0) * onehot, axis=1) - 1
    slot_index = flat_routes * capacity + position
    slot_owner = (
        jnp.full((expert_count * capacity,), -1, jnp.int32)
        .at[slot_index]
        .set(jnp.arange(flat_routes.shape[0], dtype=jnp.int32))
    )
    is_used = slot_owner >= 0
    safe_owner = jnp.where(is_used, slot_owner, 0)
    token_index = safe_owner // top_k
    slot_gates = jnp.where(
        is_used, gate_weights.reshape(-1)[safe_owner], jnp.zeros((), jnp.bfloat16)
    )
    slot_gates = slot_gates.reshape(expert_count, capacity)

    def gather_slots(source):
        picked_rows = jnp.where(is_used[:, None], source[token_index], jnp.zeros((), jnp.bfloat16))
        return picked_rows.reshape(expert_count, capacity, source.shape[1])

    col_width = model_width // lax.axis_size("tp")
    col_start = lax.axis_index("tp") * col_width
    token_cols = lax.dynamic_slice_in_dim(tokens, col_start, col_width, 1)
    cot_cols = lax.dynamic_slice_in_dim(cotangent, col_start, col_width, 1)
    rows_part, cots_part, gates_in = (
        lax.all_to_all(gather_slots(token_cols), "ep", split_axis=0, concat_axis=0, tiled=True),
        lax.all_to_all(gather_slots(cot_cols), "ep", split_axis=0, concat_axis=0, tiled=True),
        lax.all_to_all(slot_gates, "ep", split_axis=0, concat_axis=0, tiled=True),
    )
    in_rows, cot_in = (
        lax.all_gather(rows_part, "tp", axis=2, tiled=True),
        lax.all_gather(cots_part, "tp", axis=2, tiled=True),
    )
    slot_count = in_rows.shape[0] * in_rows.shape[1]
    grad_in, gate_part, grad_gate, grad_upw, grad_down = expert_backward(
        in_rows.reshape(slot_count, model_width),
        cot_in.reshape(slot_count, model_width),
        gates_in.reshape(slot_count, 1).astype(jnp.float32),
        gate_proj[0],
        up_proj[0],
        down_proj[0],
    )
    gate_total = lax.psum(gate_part, "tp")
    grad_cols = lax.psum_scatter(
        grad_in.astype(jnp.bfloat16), "tp", scatter_dimension=1, tiled=True
    ).astype(jnp.float32)
    back_rows, back_gates = (
        lax.all_to_all(
            grad_cols.reshape(expert_count, capacity, grad_cols.shape[1]).astype(jnp.bfloat16),
            "ep",
            split_axis=0,
            concat_axis=0,
            tiled=True,
        ).astype(jnp.float32),
        lax.all_to_all(
            gate_total.reshape(expert_count, capacity).astype(jnp.bfloat16),
            "ep",
            split_axis=0,
            concat_axis=0,
            tiled=True,
        ).astype(jnp.float32),
    )
    picked = back_rows.reshape(expert_count * capacity, back_rows.shape[2])[slot_index]
    grad_tokens = jnp.sum(picked.reshape(tok_rows, top_k, picked.shape[1]), axis=1).astype(
        jnp.bfloat16
    )
    grad_gates = back_gates.reshape(-1)[slot_index].reshape(tok_rows, top_k)
    return (grad_tokens, grad_gates, grad_gate[None], grad_upw[None], grad_down[None])


MESH = pl.DeviceIdType.MESH
F32, BF16 = jnp.float32, jnp.bfloat16
NT = (((1,), (1,)), ((), ()))
TN = (((0,), (0,)), ((), ()))


def flip(index, mask):
    if mask & 1:
        index = index + 1 - 2 * (index % 2)
    if mask & 2:
        index = index + 2 - 4 * ((index // 2) % 2)
    if mask & 4:
        index = index + 4 - 8 * ((index // 4) % 2)
    return index


def lanes(start, size, unit=128):
    return pl.ds(pl.multiple_of(start, unit), size)


class Copies:
    def __init__(self, send_sem, recv_sem):
        self.send_sem, self.recv_sem, self.made = send_sem, recv_sem, []

    def send(self, src, dst, ep, tp):
        n = len(self.made)
        copy = pltpu.make_async_remote_copy(
            src_ref=src,
            dst_ref=dst,
            send_sem=self.send_sem.at[n],
            recv_sem=self.recv_sem.at[n],
            device_id=(ep, tp),
            device_id_type=MESH,
        )
        copy.start()
        self.made.append(copy)
        return copy

    def finish(self):
        for copy in self.made:
            copy.wait_send()


def layer_kernel(
    tok, cot, routing, gates, w_gate, w_up, w_down,
    out, gates_out, d_gate, d_up, d_down,
    routes_in, weight_in, x, c, scaled, wcat, wd, pu, hcat, hid, part,
    gs, gin, gcol, gacc, r1, m, r2, r4, s, r3, gp, rg, gt, go,
    send_sem, recv_sem, own_sem,
):
    me, t = lax.axis_index("ep"), lax.axis_index("tp")
    core, z = t % 2, t // 2
    rows, width = tok.shape
    units = w_gate.shape[1]
    full_tiles = units // 256
    size = out.shape[1]
    eighth = width // 8
    quarter = 2 * eighth
    chunk = 2 * size
    q, far = t % 4, flip(t % 4, 2)
    other = flip(t, 1)
    blocks = {j: pl.ds(j * rows, rows) for j in range(4)}

    n = 0
    loads = []
    for src, dst in (
        (tok, x.at[blocks[0]]),
        (cot, c.at[blocks[0]]),
        (routing, routes_in),
        (gates, weight_in),
    ):
        loads.append(pltpu.make_async_copy(src, dst, own_sem.at[n]))
        n += 1
    weights = []
    for k in range(units // 128):
        for a, w in enumerate((w_gate, w_up)):
            weights.append(
                pltpu.make_async_copy(
                    w.at[:, pl.ds(128 * k, 128)],
                    wcat.at[:, pl.ds(256 * k + 128 * a, 128)],
                    own_sem.at[n],
                )
            )
            n += 1
    weights.append(pltpu.make_async_copy(w_down, wd, own_sem.at[n]))
    for copy in loads:
        copy.start()

    barrier = pltpu.get_barrier_semaphore()
    partners = [(flip(me, j), t) for j in (1, 2, 3)] + [(me, flip(t, k)) for k in (1, 2, 4, 6)]
    for device in partners:
        pl.semaphore_signal(barrier, inc=1, device_id=device, device_id_type=MESH)

    gs[...] = jnp.zeros_like(gs)
    gacc[...] = jnp.zeros_like(gacc)
    for copy in loads:
        copy.wait()
    for copy in weights:
        copy.start()
    routes, weight = routes_in[...], weight_in[...].astype(F32)
    for j in range(4):
        row = jnp.sum(jnp.where(routes == flip(me, j), weight, 0.0), axis=0, keepdims=True)
        gs[j, :, 0:rows] = jnp.broadcast_to(row, (8, rows))
    pl.semaphore_wait(barrier, len(partners))

    do = Copies(send_sem, recv_sem)
    gate_in = [do.send(gs.at[j], gin.at[j], flip(me, j), t) for j in (1, 2, 3)]

    def ep_send(a, j, cols):
        ref = both[a]
        copy = do.send(ref.at[blocks[0], cols], ref.at[blocks[j], cols], flip(me, j), t)
        return (copy, a, j, cols)

    def relay(item, mask):
        piece = both[item[1]].at[blocks[item[2]], item[3]]
        return do.send(piece, piece, me, flip(t, mask))

    low, high = lanes(quarter * q, eighth), lanes(quarter * q + eighth, eighth)
    far_low, far_high = lanes(quarter * far, eighth), lanes(quarter * far + eighth, eighth)
    both = (x, c)
    lead, rest, wide = {}, {}, {}
    landed = {0: [], 1: [], 2: [], 3: []}

    def over_ep(item, j):
        _, a, _, cols = item
        src = both[a].at[blocks[item[2]], cols]
        copy = do.send(src, both[a].at[blocks[3], cols], flip(me, j), t)
        return (copy, a, 3, cols)

    def over_z(item, mirror):
        return (relay(item, 2), item[1], item[2], mirror)

    def pass_on(items):
        for item in items:
            item[0].wait_recv()
            landed[item[2]].append((item[1], relay(item, 1)))

    def complete(j, a):
        for kind, copy in landed[j]:
            if kind == a:
                copy.wait_recv()

    lead[0] = [ep_send(0, 1, low), ep_send(0, 2, high)]
    rest[0] = [ep_send(0, 1, high), ep_send(0, 2, low)]
    wide[0] = [ep_send(0, 1, far_high), ep_send(0, 2, far_low)]

    def gate_up(at, count):
        def tile(start, size_of):
            cols = lanes(start, size_of, 256)
            pu[at, cols] = jnp.dot(x[at, :], wcat[:, cols], preferred_element_type=F32)

        def body(k, carry):
            tile(512 * k, 512)
            return carry

        lax.fori_loop(0, full_tiles, body, 0, unroll=True)
        if units % 256:
            tile(512 * full_tiles, 256)

    def back_of(at, js):
        def tile(start, size_of):
            unit = lanes(start, size_of)
            back_all = lax.dot_general(c[at, :], wd[unit, :], NT, preferred_element_type=F32)
            for n, j in enumerate(js):
                mine = slice(n * rows, (n + 1) * rows)
                g = gcol[j]
                total = gacc[j, 0:rows, :]
                for k in range(size_of // 128):
                    pre = pu[blocks[j], lanes(2 * start + 256 * k, 128)]
                    up = pu[blocks[j], lanes(2 * start + 256 * k + 128, 128)]
                    back = back_all[mine, 128 * k : 128 * k + 128]
                    sig = jax.nn.sigmoid(pre)
                    act = pre * sig
                    hidden = (act * up).astype(BF16)
                    total = total + hidden.astype(F32) * back
                    scaled_back = g * back
                    grad_pre = scaled_back * up * sig * (1.0 + pre * (1.0 - sig))
                    hid[blocks[j], lanes(start + 128 * k, 128)] = hidden
                    hcat[blocks[j], lanes(2 * start + 256 * k, 128)] = grad_pre.astype(BF16)
                    hcat[blocks[j], lanes(2 * start + 256 * k + 128, 128)] = (
                        scaled_back * act
                    ).astype(BF16)
                gacc[j, 0:rows, :] = total

        def body(k, carry):
            tile(256 * k, 256)
            return carry

        lax.fori_loop(0, full_tiles, body, 0, unroll=True)
        if units % 256:
            tile(256 * full_tiles, 128)

    def scale(j):
        g = gcol[j][:, 0:1]
        scaled[blocks[j], :] = (g * c[blocks[j], :].astype(F32)).astype(BF16)

    def column(j, tile):
        gcol[j] = jnp.broadcast_to(tile.T[0:rows, 0:1], (rows, 128))

    base = 64

    def first(i, j):
        d = (z + 1 + i) % 4
        return pltpu.make_async_remote_copy(
            src_ref=part.at[blocks[j], lanes(chunk * d + size * (1 - core), size)],
            dst_ref=r1.at[4 * d + j],
            send_sem=send_sem.at[base + 4 * i + j],
            recv_sem=recv_sem.at[base + 4 * i + j],
            device_id=(me, other),
            device_id_type=MESH,
        )

    def second(i, j):
        d = (z + 1 + i) % 4
        return pltpu.make_async_remote_copy(
            src_ref=m.at[4 * d + j],
            dst_ref=r2.at[4 * d + j],
            send_sem=send_sem.at[base + 16 + 4 * i + j],
            recv_sem=recv_sem.at[base + 16 + 4 * i + j],
            device_id=(flip(me, j), t),
            device_id_type=MESH,
        )

    def fourth(d):
        return pltpu.make_async_remote_copy(
            src_ref=m.at[4 * d + 3],
            dst_ref=r4.at[d // 2],
            send_sem=send_sem.at[base + 36 + d],
            recv_sem=recv_sem.at[base + 36 + d],
            device_id=(me, flip(t, 2)),
            device_id_type=MESH,
        )

    def send_diagonal():
        for i in (1, 3):
            d = (z + 1 + i) % 4
            fourth(d).wait_recv()
            m[4 * d + 3] = (m[4 * d + 3].astype(F32) + r4[d // 2].astype(F32)).astype(BF16)
            second(i, 3).start()

    def merge(i, j):
        d = (z + 1 + i) % 4
        first(i, j).wait_recv()
        mine = part[blocks[j], lanes(chunk * d + size * core, size)].astype(F32)
        m[4 * d + j] = (mine + r1[4 * d + j].astype(F32)).astype(BF16)
        if j == 3 and i % 2 == 0:
            fourth(d).start()
        elif j in (1, 2):
            second(i, j).start()

    def grad_in(at, js, merged=(), step=None, hook=None):
        for i in range(4):
            d = (z + 1 + i) % 4
            cols = lanes(chunk * d, chunk, 256)
            part[at, cols] = lax.dot_general(
                hcat[at, :], wcat[cols, :], NT, preferred_element_type=F32
            ).astype(BF16)
            for j in js:
                first(i, j).start()
            if i:
                for j in merged:
                    merge(i - 1, j)
            if i == step:
                hook()
        for j in merged:
            merge(3, j)

    def d_hidden(lo, hi):
        def body(i, carry):
            cols = lanes(256 * i, 256, 256)
            grads = lax.dot_general(
                x[:, cols], hcat[...], TN, preferred_element_type=F32
            ).astype(BF16)
            for k in range(units // 128):
                d_gate[cols, 128 * k : 128 * k + 128] = grads[:, 256 * k : 256 * k + 128]
                d_up[cols, 128 * k : 128 * k + 128] = grads[:, 256 * k + 128 : 256 * k + 256]
            return carry

        lax.fori_loop(lo, hi, body, 0, unroll=2)

    def d_out(lo, hi):
        def body(i, carry):
            cols = lanes(128 * i, 128)
            d_down[cols, :] = lax.dot_general(
                hid[:, cols], scaled[...], TN, preferred_element_type=F32
            ).astype(BF16)
            return carry

        lax.fori_loop(lo, hi, body, 0, unroll=2)

    column(0, gs[0])
    for copy in weights:
        copy.wait()
    gate_up(blocks[0], 1)
    pass_on(lead[0])
    diag = {0: [over_ep(lead[0][0], 2), over_ep(lead[0][1], 1)]}
    crossed = {0: [over_z(lead[0][0], far_low), over_z(lead[0][1], far_high)]}
    lead[1] = [ep_send(1, 1, low), ep_send(1, 2, high)]
    wide[1] = [ep_send(1, 1, far_high), ep_send(1, 2, far_low)]
    rest[1] = [ep_send(1, 1, high), ep_send(1, 2, low)]
    back_of(blocks[0], (0,))
    pass_on(rest[0])
    pass_on(wide[0])
    grad_in(blocks[0], (0,), (0,))
    pass_on(crossed[0])
    pass_on(diag[0])
    across = {0: [over_z(diag[0][0], far_low), over_z(diag[0][1], far_high)]}
    for copy in gate_in:
        copy.wait_recv()
    for j in (1, 2, 3):
        column(j, gin[j])
    scale(0)
    pass_on(lead[1])
    diag[1] = [over_ep(lead[1][0], 2), over_ep(lead[1][1], 1)]
    crossed[1] = [over_z(lead[1][0], far_low), over_z(lead[1][1], far_high)]
    complete(1, 0)
    complete(2, 0)
    pair = pl.ds(rows, 2 * rows)
    gate_up(pair, 2)
    pass_on(wide[1])
    diag[1] += [over_ep(wide[1][0], 2), over_ep(wide[1][1], 1)]
    pass_on(rest[1])
    pass_on(across[0])
    complete(3, 0)
    gate_up(blocks[3], 1)
    pass_on(crossed[1][0:1])
    complete(1, 1)
    back_of(blocks[1], (1,))
    pass_on(diag[1])
    pass_on(crossed[1][1:2])
    complete(3, 1)
    back_of(blocks[3], (3,))
    grad_in(blocks[3], (3,), (3,))
    complete(2, 1)
    back_of(blocks[2], (2,))
    grad_in(pair, (1, 2), (1, 2), 2, send_diagonal)
    for j in (1, 2, 3):
        scale(j)
    for j in range(4):
        row = jnp.sum(gacc[j].T, axis=0, keepdims=True)
        gp[j] = jnp.broadcast_to(row, gp.shape[1:])
    stage = do.send(gp, rg.at[0], me, other)
    d_out(0, 4)

    def gathered(i):
        d = (z + 1 + i) % 4
        total = m[4 * d].astype(F32)
        for j in (3, 1, 2) if i % 2 else (1, 2):
            second(i, j).wait_recv()
            total = total + r2[4 * d + j].astype(F32)
        return total

    def third(i):
        d = (z + 1 + i) % 4
        return pltpu.make_async_remote_copy(
            src_ref=s.at[d],
            dst_ref=r3.at[i],
            send_sem=send_sem.at[base + 32 + i],
            recv_sem=recv_sem.at[base + 32 + i],
            device_id=(me, 2 * d + core),
            device_id_type=MESH,
        )

    def pass_third(i):
        s[(z + 1 + i) % 4] = gathered(i).astype(BF16)
        third(i).start()

    stage.wait_recv()
    gt[0] = gp[...] + rg[0]
    stage = do.send(gt.at[0], rg.at[1], me, flip(t, 2))
    pass_third(0)
    d_out(4, units // 128)
    stage.wait_recv()
    gt[1] = gt[0] + rg[1]
    stage = do.send(gt.at[1], rg.at[2], me, flip(t, 4))
    pass_third(1)
    d_hidden(0, width // 1024)
    stage.wait_recv()
    gt[2] = gt[1] + rg[2]
    gate_back = [do.send(gt.at[2, j], go.at[j], flip(me, j), t) for j in (1, 2, 3)]
    pass_third(2)
    d_hidden(width // 1024, width // 512)
    total = gathered(3)
    d_hidden(width // 512, width // 256)
    for copy in gate_back:
        copy.wait_recv()
    sums = [gt[2, 0]] + [go[j] for j in (1, 2, 3)]
    picked = jnp.zeros(routing.shape, F32)
    for j in range(4):
        row = jnp.broadcast_to(sums[j][0:1, 0:rows], routing.shape)
        picked = jnp.where(routes == flip(me, j), row, picked)
    gates_out[...] = picked
    for i in range(3):
        third(i).wait_recv()
        total = total + r3[i].astype(F32)
    out[...] = total.astype(out.dtype)
    do.finish()
    for i in range(4):
        for j in range(4):
            first(i, j).wait_send()
            if j in (1, 2) or (j and i % 2):
                second(i, j).wait_send()
        if i % 2 == 0:
            fourth((z + 1 + i) % 4).wait_send()
        if i < 3:
            third(i).wait_send()


def store_kernel(*refs):
    sources, targets, sem = refs[0:5], refs[5:10], refs[10]
    copies = []
    for a, (src, dst) in enumerate(zip(sources, targets)):
        parts = 4 if src.shape[0] % 512 == 0 or src.shape[0] > 512 else 1
        step = src.shape[0] // parts
        for k in range(parts):
            piece = pl.ds(k * step, step)
            copies.append(pltpu.make_async_copy(src.at[piece], dst.at[piece], sem.at[a, k]))
    for copy in copies:
        copy.start()
    for copy in copies:
        copy.wait()


def dense(tokens, cotangent, routing, gate_weights, gate_proj, up_proj, down_proj):
    rows, width = tokens.shape
    units, parts = gate_proj.shape[2], lax.axis_size("tp")
    size = width // parts
    top_k = routing.shape[1]
    vmem, hbm = pl.BlockSpec(memory_space=pltpu.VMEM), pl.BlockSpec(memory_space=pltpu.HBM)
    shape = jax.ShapeDtypeStruct
    tile = pltpu.VMEM((16, rows, size), BF16)
    flat = (4, 8, 256)
    results = pl.pallas_call(
        layer_kernel,
        out_shape=[
            pltpu.VMEM((rows, size), BF16),
            pltpu.VMEM((top_k, rows), F32),
            pltpu.VMEM((width, units), BF16),
            pltpu.VMEM((width, units), BF16),
            pltpu.VMEM((units, width), BF16),
        ],
        in_specs=[hbm] * 7,
        out_specs=[vmem] * 5,
        scratch_shapes=[
            pltpu.VMEM((top_k, rows), routing.dtype),
            pltpu.VMEM((top_k, rows), gate_weights.dtype),
            pltpu.VMEM((4 * rows, width), BF16),
            pltpu.VMEM((4 * rows, width), BF16),
            pltpu.VMEM((4 * rows, width), BF16),
            pltpu.VMEM((width, 2 * units), BF16),
            pltpu.VMEM((units, width), BF16),
            pltpu.VMEM((4 * rows, 2 * units), F32),
            pltpu.VMEM((4 * rows, 2 * units), BF16),
            pltpu.VMEM((4 * rows, units), BF16),
            pltpu.VMEM((4 * rows, width), BF16),
            pltpu.VMEM(flat, F32),
            pltpu.VMEM(flat, F32),
            pltpu.VMEM((4, rows, 128), F32),
            pltpu.VMEM((4, 256, 128), F32),
            tile,
            tile,
            tile,
            pltpu.VMEM((2, rows, size), BF16),
            pltpu.VMEM((4, rows, size), BF16),
            pltpu.VMEM((3, rows, size), BF16),
            pltpu.VMEM(flat, F32),
            pltpu.VMEM((3,) + flat, F32),
            pltpu.VMEM((3,) + flat, F32),
            pltpu.VMEM(flat, F32),
            pltpu.SemaphoreType.DMA((104,)),
            pltpu.SemaphoreType.DMA((104,)),
            pltpu.SemaphoreType.DMA((5 + 2 * (units // 128),)),
        ],
        compiler_params=pltpu.CompilerParams(
            collective_id=0, has_side_effects=True, vmem_limit_bytes=42 << 20
        ),
    )(
        *(
            pltpu.with_memory_space_constraint(a, pltpu.HBM)
            for a in (
                tokens,
                cotangent,
                routing.T,
                gate_weights.T,
                gate_proj[0],
                up_proj[0],
                down_proj[0],
            )
        )
    )
    grad_tokens, grad_gates, d_gate, d_up, d_down = pl.pallas_call(
        store_kernel,
        out_shape=[shape(r.shape, r.dtype) for r in results],
        in_specs=[vmem] * 5,
        out_specs=[hbm] * 5,
        scratch_shapes=[pltpu.SemaphoreType.DMA((5, 4))],
        compiler_params=pltpu.CompilerParams(vmem_limit_bytes=1 << 20),
    )(*results)
    return grad_tokens, grad_gates.T, d_gate[None], d_up[None], d_down[None]


def local(tokens, cotangent, routing, gate_weights, gate_proj, up_proj, down_proj):
    experts, parts = lax.axis_size("ep"), lax.axis_size("tp")
    capacity = 2 * tokens.shape[0] * routing.shape[1] // experts
    fits = experts == 4 and parts == 8 and tokens.shape[1] % 1024 == 0
    fits = fits and tokens.shape[0] % 16 == 0 and tokens.shape[0] <= 256
    fits = fits and gate_proj.shape[2] % 128 == 0
    plan = dense if capacity >= tokens.shape[0] and fits else slotted
    return plan(tokens, cotangent, routing, gate_weights, gate_proj, up_proj, down_proj)


def solution(mesh):
    return jax.shard_map(
        local,
        mesh=mesh,
        in_specs=(
            P("ep", None),
            P("ep", None),
            P("ep", None),
            P("ep", None),
            P("ep", None, "tp"),
            P("ep", None, "tp"),
            P("ep", "tp", None),
        ),
        out_specs=(
            P("ep", "tp"),
            P("ep", None),
            P("ep", None, "tp"),
            P("ep", None, "tp"),
            P("ep", "tp", None),
        ),
        check_vma=False,
    )
```
